32 devices in a mesh: grp: 2 (over y), fs: 4 (over z), tp: 4 (over x, core).
Axes of the slice: x: 2, y: 2, z: 4, core: 2. Of those that a mesh axis runs over, the one named last changes fastest.
Arguments:
- layer_input: bfloat16 [3072, 2048], P(('grp', 'fs'), 'tp'), parts along dimension 0, may hold values from -6 to 6
- first_gain: bfloat16 [1, 2048], P(None, 'tp'), may hold values from 0.099609375 to 1.8984375
- ffn_gate_w: bfloat16 [2048, 6144], P('fs', 'tp'), may hold values from -0.125 to 0.125
- ffn_up_w: bfloat16 [2048, 6144], P('fs', 'tp'), may hold values from -0.125 to 0.125
- ffn_down_w: bfloat16 [6144, 2048], P('tp', 'fs'), may hold values from -0.078125 to 0.078125
- mixer_gain: bfloat16 [1, 2048], P(None, 'tp'), may hold values from 0.099609375 to 1.8984375
- pool_in_w: bfloat16 [2048, 1024], P('fs', 'tp'), may hold values from -0.125 to 0.125
- mixer_gate_w: bfloat16 [2048, 2048], P('fs', 'tp'), may hold values from -0.125 to 0.125
- group_mix_w: bfloat16 [8, 128, 128], P('tp'), may hold values from -0.5 to 0.5
- pool_scale: float32 [1, 1024], P(None, 'tp'), may hold values from 0.1 to 1.9
- mixer_out_w: bfloat16 [1024, 2048], P('tp', 'fs'), may hold values from -0.1875 to 0.1875
- second_gain: bfloat16 [1, 2048], P(None, 'tp'), may hold values from 0.099609375 to 1.8984375
Outputs:
- layer_output: bfloat16 [3072, 2048], P(('grp', 'fs'), 'tp'), parts along dimension 0
The draws below stay inside these ranges and needn't reach their ends.
There are 2 independent parts, one for each index of `grp`. The reference program is written for one: setup_inputs(seed, part) draws one part's arguments, and reference() takes and returns one part's arrays. A program takes and returns all parts, laid end to end along the dimension named above; an argument that names none is the same for every part. Nothing has to cross between parts.
All inputs are finite; a program needn't handle non-finite values.
Results may differ from the reference program's by a relative error of at most 0.015.
Values may be sent and summed in bfloat16 or wider, within the bound.
No kernel may reach another device: no remote copies, remote signals or barrier semaphores. Data moves between devices by JAX's collectives and lax.ppermute only.
A program may use at most 64 MiB of HBM per device.

```python
import jax
import jax.numpy as jnp
from jax import lax

D = 2048
FF = 6144
BW = 1024
GW = 128
GROUPS = 8
TOK_DEV = 384
TOKENS = 1536
N_FS = 4
N_TP = 4


def steps_of(key, dims, split, low, top_value):
    factor_of = 1.0
    for position, shards_of in split:
        draws = jax.random.uniform(jax.random.fold_in(jax.random.fold_in(key, 6), position), (shards_of,), jnp.float32, low / len(split), top_value / len(split))
        factor_of = factor_of * jnp.repeat(jnp.exp(draws), dims[position] // shards_of).reshape((-1,) + (1,) * (len(dims) - 1 - position))
    return factor_of


def noise(rng, extent, scale, bound, shards=(), kind=jnp.bfloat16):
    drawn = jax.random.normal(rng, extent, jnp.float32) * scale
    if len(shards) > 0:
        drawn = steps_of(rng, extent, shards, -0.22, 0.18) * drawn
    return jnp.clip(drawn, min=-bound, max=bound).astype(kind)


def setup_inputs(seed: int = 0, part: int = 0) -> dict:
    splits = jax.random.split(jax.random.key(seed), 13)
    part_keys = jax.random.split(jax.random.fold_in(splits[12], part), 13)
    layer_input = noise(part_keys[0], (TOKENS, D), 1.0, 6.0, ((0, 4), (1, 4)))
    first_gain = jnp.clip(1.0 + 0.18 * jax.random.normal(splits[1], (1, D), jnp.float32), 0.099609375, 1.8984375).astype(jnp.bfloat16)
    ffn_gate_w = noise(splits[2], (D, FF), D ** -0.5, 0.125, ((0, 4), (1, 4)))
    ffn_up_w = noise(splits[3], (D, FF), D ** -0.5, 0.125, ((0, 4), (1, 4)))
    ffn_down_w = noise(splits[4], (FF, D), FF ** -0.5, 0.078125, ((0, 4), (1, 4)))
    mixer_gain = jnp.clip(1.0 + 0.18 * jax.random.normal(splits[5], (1, D), jnp.float32), 0.099609375, 1.8984375).astype(jnp.bfloat16)
    pool_in_w = noise(splits[6], (D, BW), D ** -0.5, 0.125, ((0, 4), (1, 4)))
    mixer_gate_w = noise(splits[7], (D, D), D ** -0.5, 0.125, ((0, 4), (1, 4)))
    group_mix_w = noise(splits[8], (GROUPS, GW, GW), GW ** -0.5, 0.5, ((0, 4),))
    pool_scale = jnp.clip(1.0 + 0.18 * jax.random.normal(splits[9], (1, BW), jnp.float32), 0.1, 1.9)
    mixer_out_w = noise(splits[10], (BW, D), BW ** -0.5, 0.1875, ((0, 4), (1, 4)))
    second_gain = jnp.clip(1.0 + 0.18 * jax.random.normal(splits[11], (1, D), jnp.float32), 0.099609375, 1.8984375).astype(jnp.bfloat16)
    return dict(layer_input=layer_input, first_gain=first_gain, ffn_gate_w=ffn_gate_w, ffn_up_w=ffn_up_w, ffn_down_w=ffn_down_w, mixer_gain=mixer_gain, pool_in_w=pool_in_w, mixer_gate_w=mixer_gate_w, group_mix_w=group_mix_w, pool_scale=pool_scale, mixer_out_w=mixer_out_w, second_gain=second_gain)


def norm_rows(values, gain):
    widened = values.astype(jnp.float32)
    scaled = (widened * gain.astype(jnp.float32)).astype(jnp.bfloat16)
    factor = lax.rsqrt(lax.optimization_barrier(jnp.mean(widened * widened, axis=1, keepdims=True)) + 1e-06)
    return (scaled, factor)

def block_sum(left, right):
    width = left.shape[1] // N_TP
    total = jnp.zeros((left.shape[0], right.shape[1]), jnp.float32)
    for block in range(N_TP):
        partial_value = jnp.dot(left[:, block * width:(block + 1) * width], right[block * width:(block + 1) * width], preferred_element_type=jnp.float32)
        rounded = lax.optimization_barrier(partial_value.astype(jnp.bfloat16))
        total = total + rounded.astype(jnp.float32)
    return total

def feed_forward(values, gain, ffn_gate_w, ffn_up_w, ffn_down_w):
    scaled, factor = norm_rows(values, gain)
    gate_pre = factor * jnp.dot(scaled, ffn_gate_w, preferred_element_type=jnp.float32)
    up_pre = factor * jnp.dot(scaled, ffn_up_w, preferred_element_type=jnp.float32)
    hidden = (jax.nn.silu(gate_pre) * up_pre).astype(jnp.bfloat16)
    return block_sum(hidden, ffn_down_w)

def reference(layer_input, first_gain, ffn_gate_w, ffn_up_w, ffn_down_w, mixer_gain, pool_in_w, mixer_gate_w, group_mix_w, pool_scale, mixer_out_w, second_gain):
    first = (layer_input.astype(jnp.float32) + 0.5 * feed_forward(layer_input, first_gain, ffn_gate_w, ffn_up_w, ffn_down_w)).astype(jnp.bfloat16)
    scaled, factor = norm_rows(first, mixer_gain)
    pool_pre = (factor * jnp.dot(scaled, pool_in_w, preferred_element_type=jnp.float32)).astype(jnp.bfloat16)
    gate_logit = factor * jnp.dot(scaled, mixer_gate_w, preferred_element_type=jnp.float32)
    values = pool_pre.astype(jnp.float32).reshape(N_FS, TOK_DEV, GROUPS, GW)
    running = jnp.cumsum(values, axis=1)
    positions = jnp.arange(TOK_DEV, dtype=jnp.int32)
    windows = 2 ** (1 + jnp.arange(GROUPS, dtype=jnp.int32) % 4)
    chosen = jnp.zeros_like(values)
    for span in (2, 4, 8, 16):
        lagged = jnp.pad(running, ((0, 0), (span, 0), (0, 0), (0, 0)))[:, :TOK_DEV]
        counts = jnp.minimum(positions + 1, span).astype(jnp.float32)[None, :, None, None]
        means = (running - lagged) / counts
        chosen = jnp.where((windows == span)[None, None, :, None], means, chosen)
    trail = (chosen - values).astype(jnp.bfloat16)
    mixed = jnp.einsum('ntgc,gcd->ntgd', trail.astype(jnp.float32), group_mix_w.astype(jnp.float32))
    pooled = (mixed.reshape(TOKENS, BW) * pool_scale).astype(jnp.bfloat16)
    lifted = block_sum(pooled, mixer_out_w)
    second = (first.astype(jnp.float32) + jax.nn.sigmoid(gate_logit) * lifted).astype(jnp.bfloat16)
    result = second.astype(jnp.float32) + 0.5 * feed_forward(second, second_gain, ffn_gate_w, ffn_up_w, ffn_down_w)
    return result.astype(jnp.bfloat16)
```

```python
import jax
import jax.numpy as jnp
from jax import lax
from jax.sharding import PartitionSpec as P


def shift(size, step):
    return [(i, (i + step) % size) for i in range(size)]


def swap(size):
    return [(i, i ^ 1) for i in range(size)]


def per_device(
    layer_input,
    first_gain,
    ffn_gate_w,
    ffn_up_w,
    ffn_down_w,
    mixer_gain,
    pool_in_w,
    mixer_gate_w,
    group_mix_w,
    pool_scale,
    mixer_out_w,
    second_gain,
):
    n_grp, n_fs, n_tp = (lax.axis_size(name) for name in ("grp", "fs", "tp"))
    n_chip = n_tp // 2
    y, z, t = (lax.axis_index(name) for name in ("grp", "fs", "tp"))
    chip, core = t // 2, t % 2
    rows, shard = layer_input.shape
    width = shard * n_tp
    block = width // n_fs

    def pieces_of(weight, axis):
        part = weight.shape[axis] // n_grp
        own = [
            lax.dynamic_slice_in_dim(weight, ((y - k) % n_grp) * part, part, axis)
            for k in range(n_grp)
        ]
        gathered, current = [own], own[0]
        for _ in range(n_fs - 1):
            current = lax.ppermute(current, "fs", shift(n_fs, 1))
            gathered.append(
                [current] + [lax.ppermute(current, "grp", shift(n_grp, k)) for k in range(1, n_grp)]
            )
        return gathered

    def absolute(weight, axis, split):
        gathered = pieces_of(weight, split)
        shape = list(weight.shape)
        shape[axis] *= n_fs
        whole = jnp.zeros(shape, weight.dtype)
        for s, parts in enumerate(gathered):
            for k, part in enumerate(parts):
                start = [0, 0]
                start[axis] = ((z - s) % n_fs) * weight.shape[axis]
                start[split] = start[split] + ((y - k) % n_grp) * part.shape[split]
                whole = lax.dynamic_update_slice(whole, part, start)
        return whole

    def gather_tp(value):
        pieces = [(t, value), (t ^ 1, lax.ppermute(value, "tp", swap(n_tp)))]
        for k in range(1, n_chip):
            far = lax.ppermute(value, "tp", shift(n_tp, 2 * k))
            source = (t - 2 * k) % n_tp
            pieces.append((source, far))
            pieces.append((source ^ 1, lax.ppermute(far, "tp", swap(n_tp))))
        whole = jnp.zeros((value.shape[0], value.shape[1] * n_tp), value.dtype)
        for source, piece in pieces:
            whole = lax.dynamic_update_slice(whole, piece, (0, source * value.shape[1]))
        return whole

    def scatter_tp(partial):
        def at(index):
            return lax.dynamic_slice_in_dim(partial, index * shard, shard, 1)

        total = None
        for k in list(range(1, n_chip)) + [0]:
            there = ((chip + k) % n_chip) * 2
            other = lax.ppermute(at(there + (1 - core)), "tp", swap(n_tp))
            pair = at(there + core).astype(jnp.float32) + other.astype(jnp.float32)
            if k:
                pair = lax.ppermute(
                    pair.astype(jnp.bfloat16), "tp", shift(n_tp, 2 * k)
                ).astype(jnp.float32)
            total = pair if total is None else total + pair
        return total

    def norm_rows(values, gain):
        whole = gather_tp(values)
        gain_whole = lax.all_gather(gain, "tp", axis=1, tiled=True)
        widened = whole.astype(jnp.float32)
        scaled = (widened * gain_whole.astype(jnp.float32)).astype(jnp.bfloat16)
        factor = lax.rsqrt(jnp.mean(widened * widened, axis=1, keepdims=True) + 1e-06)
        return scaled, factor

    gate_pieces = pieces_of(ffn_gate_w, 1)
    up_pieces = pieces_of(ffn_up_w, 1)
    down_pieces = pieces_of(ffn_down_w, 0)

    def feed_forward(values, gain):
        scaled, factor = norm_rows(values, gain)
        inputs = [
            lax.dynamic_slice_in_dim(scaled, ((z - s) % n_fs) * block, block, 1)
            for s in range(n_fs)
        ]

        def project(gathered, k):
            total = None
            for s in range(n_fs):
                product = jnp.dot(inputs[s], gathered[s][k], preferred_element_type=jnp.float32)
                total = product if total is None else total + product
            return total

        hidden = [
            (
                jax.nn.silu(factor * project(gate_pieces, k)) * (factor * project(up_pieces, k))
            ).astype(jnp.bfloat16)
            for k in range(n_grp)
        ]
        out = jnp.zeros((rows, width), jnp.bfloat16)
        for s in range(n_fs):
            product = None
            for k in range(n_grp):
                term = jnp.dot(hidden[k], down_pieces[s][k], preferred_element_type=jnp.float32)
                product = term if product is None else product + term
            out = lax.dynamic_update_slice(
                out, product.astype(jnp.bfloat16), (0, ((z - s) % n_fs) * block)
            )
        return scatter_tp(out)

    first = (
        layer_input.astype(jnp.float32) + 0.5 * feed_forward(layer_input, first_gain)
    ).astype(jnp.bfloat16)

    pool_in = absolute(pool_in_w, 0, 0)
    mixer_gate = absolute(mixer_gate_w, 0, 0)
    mixer_out = absolute(mixer_out_w, 1, 0)
    scaled, factor = norm_rows(first, mixer_gain)
    pool_pre = (
        factor * jnp.dot(scaled, pool_in, preferred_element_type=jnp.float32)
    ).astype(jnp.bfloat16)
    gate_logit = factor * jnp.dot(scaled, mixer_gate, preferred_element_type=jnp.float32)
    groups, group_width = group_mix_w.shape[:2]
    position = lax.broadcasted_iota(jnp.int32, (rows, rows), 0)
    back = position - lax.broadcasted_iota(jnp.int32, (rows, rows), 1)
    row = lax.broadcasted_iota(jnp.int32, (rows, 1), 0)
    pooled = []
    for g in range(groups):
        window = 2 ** (1 + (t * groups + g) % 4)
        band = ((back >= 0) & (back < window)).astype(jnp.bfloat16)
        values = pool_pre[:, g * group_width : (g + 1) * group_width]
        sums = jnp.dot(band, values, preferred_element_type=jnp.float32)
        count = jnp.minimum(row + 1, window).astype(jnp.float32)
        trail = (sums / count - values.astype(jnp.float32)).astype(jnp.bfloat16)
        mixed = jnp.dot(trail, group_mix_w[g], preferred_element_type=jnp.float32)
        pooled.append(mixed)
    pooled = (jnp.concatenate(pooled, axis=1) * pool_scale).astype(jnp.bfloat16)
    lifted = scatter_tp(
        jnp.dot(pooled, mixer_out, preferred_element_type=jnp.float32).astype(jnp.bfloat16)
    )
    second = (first.astype(jnp.float32) + jax.nn.sigmoid(gate_logit) * lifted).astype(jnp.bfloat16)
    result = second.astype(jnp.float32) + 0.5 * feed_forward(second, second_gain)
    return result.astype(jnp.bfloat16)


def solution(mesh):
    return jax.shard_map(
        per_device,
        mesh=mesh,
        in_specs=(
            P(("grp", "fs"), "tp"),
            P(None, "tp"),
            P("fs", "tp"),
            P("fs", "tp"),
            P("tp", "fs"),
            P(None, "tp"),
            P("fs", "tp"),
            P("fs", "tp"),
            P("tp", None, None),
            P(None, "tp"),
            P("tp", "fs"),
            P(None, "tp"),
        ),
        out_specs=P(("grp", "fs"), "tp"),
        check_vma=False,
    )
```
